32 devices in a mesh: sp: 16 (over z, y, x), tp: 2 (over core).
Axes of the slice: x: 2, y: 2, z: 4, core: 2. Of those that a mesh axis runs over, the one named last changes fastest.
Arguments:
- value_in: bfloat16 [4096, 2048], P('sp', 'tp'), may hold values from -25 to 25, as said below
- gate_in: bfloat16 [4096, 2048], P('sp', 'tp'), may hold values from -6 to 6
- taps: float32 [31, 2048], P(None, 'tp'), may hold values from -1 to 1
- gain: float32 [2048], P('tp'), may hold values from 0.1 to 1.9
- shift: float32 [2048], P('tp'), may hold values from -3 to 3
- w_out: bfloat16 [2048, 2048], P('tp'), may hold values from -0.125 to 0.125
- grad_out: bfloat16 [4096, 2048], P('sp'), may hold values from -6 to 6
Outputs:
- d_value: bfloat16 [4096, 2048], P('sp', 'tp')
- d_gate: bfloat16 [4096, 2048], P('sp', 'tp')
- d_taps: float32 [31, 2048], P(None, 'tp')
- d_gain: float32 [2048], P('tp')
- d_shift: float32 [2048], P('tp')
The draws below stay inside these ranges and needn't reach their ends.
Inputs may be any that keep to these rules, and one draw needn't show every extreme that they name: `value_in`: channel blocks of different magnitude.
All inputs are finite; a program needn't handle non-finite values.
Results may differ from the reference program's by a relative error of at most 0.007.
Values may be sent and summed in bfloat16 or wider, within the bound.
A program may use at most 64 MiB of HBM per device.

```python
import math
import jax
import jax.numpy as jnp
from jax import lax

C = 2048
D = 2048
KERNEL = 31
TOK_DEV = 256
TOKENS = 4096
N_SP = 16


def draw_value_in(key, part):
    key_base = jax.random.fold_in(key, 11)
    key_group = jax.random.fold_in(key, 12)
    key_flip = jax.random.fold_in(key, 13)
    base = jnp.clip(jax.random.normal(key_base, (TOKENS, C), jnp.float32), -4.0, 4.0)
    column = jnp.exp(jax.random.uniform(key_group, (C,), jnp.float32, -0.7, 0.7))
    flip = jax.random.randint(key_flip, (), 0, 2)
    upper = (jnp.arange(C) >= C // 2).astype(jnp.int32)
    factor = jnp.where(upper == flip, 3.0, 1.0)
    return (base * column * factor).astype(jnp.bfloat16)


def shard_levels(own_key, extent, pieces, low, high):
    factor_of = 1.0
    for position, shards_of in pieces:
        heights = jax.random.uniform(jax.random.fold_in(jax.random.fold_in(own_key, 6), position), (shards_of,), jnp.float32, low / len(pieces), high / len(pieces))
        factor_of = factor_of * jnp.repeat(jnp.exp(heights), extent[position] // shards_of).reshape((-1,) + (1,) * (len(extent) - 1 - position))
    return factor_of


def noise(rng, extent, scale, most, pieces=(), kind=jnp.bfloat16):
    array = scale * jax.random.normal(rng, extent, jnp.float32)
    if pieces:
        array = array * shard_levels(rng, extent, pieces, -0.22, 0.18)
    return jnp.clip(array, -most, most).astype(kind)


def setup_inputs(seed: int = 0) -> dict:
    splits = jax.random.split(jax.random.key(seed), 8)
    return {
        "value_in": draw_value_in(jax.random.fold_in(splits[7], 71), 0),
        "gate_in": noise(splits[1], (TOKENS, C), 1.5, 6.0, ((0, 16), (1, 2))),
        "taps": noise(splits[2], (KERNEL, C), 0.18, 1.0, ((1, 2),), jnp.float32),
        "gain": jnp.clip(1.0 + 0.18 * jax.random.normal(splits[3], (C,), jnp.float32), 0.1, 1.9),
        "shift": noise(splits[4], (C,), 0.5, 3.0, ((0, 2),), jnp.float32),
        "w_out": noise(splits[5], (C, D), D ** -0.5, 0.125, ((0, 2),)),
        "grad_out": noise(splits[6], (TOKENS, D), 1.0, 6.0, ((0, 16),)),
    }


EPS = 1e-05

def convolve(window, taps, count):
    total = jnp.zeros((count, window.shape[1]), jnp.float32)
    for offset in range(taps.shape[0]):
        total = total + taps[offset] * window[offset:offset + count]
    return total

def norm_backward(conv_out, grad_rows, gain, shift, w_out):
    width = conv_out.shape[1]
    mean = lax.optimization_barrier(jnp.sum(conv_out, 1)) / width
    var = lax.optimization_barrier(jnp.sum(conv_out * conv_out, 1)) / width - mean * mean
    inv = lax.rsqrt(var + EPS)
    normed = (conv_out - mean[:, None]) * inv[:, None]
    pre = normed * gain + shift
    grad_mix = jnp.dot(grad_rows, w_out.T, preferred_element_type=jnp.float32)
    sig = jax.nn.sigmoid(pre)
    grad_pre = grad_mix * sig * (1.0 + pre * (1.0 - sig))
    grad_normed = grad_pre * gain
    first = lax.optimization_barrier(jnp.sum(grad_normed, 1)) / width
    second = lax.optimization_barrier(jnp.sum(grad_normed * normed, 1)) / width
    grad_conv = inv[:, None] * (grad_normed - first[:, None] - normed * second[:, None])
    return (grad_conv, grad_pre, normed)

def reference(value_in, gate_in, taps, gain, shift, w_out, grad_out):
    half = KERNEL // 2
    gate_sig = jax.nn.sigmoid(gate_in.astype(jnp.float32))
    gated = (value_in.astype(jnp.float32) * gate_sig).astype(jnp.bfloat16)
    gated_pad = jnp.pad(gated, ((half, half), (0, 0)))

    def first_pass(index):
        start = (index * TOK_DEV).astype(jnp.int32)
        window = lax.dynamic_slice_in_dim(gated_pad, start, TOK_DEV + 2 * half, 0).astype(jnp.float32)
        conv_out = convolve(window, taps, TOK_DEV)
        grad_rows = lax.dynamic_slice_in_dim(grad_out, start, TOK_DEV, 0)
        grad_conv, grad_pre, normed = norm_backward(conv_out, grad_rows, gain, shift, w_out)
        return (grad_conv, lax.optimization_barrier(jnp.sum(grad_pre * normed, 0)), lax.optimization_barrier(jnp.sum(grad_pre, 0)))
    blocks = jnp.arange(N_SP, dtype=jnp.int32)
    grad_conv, gain_parts, shift_parts = lax.map(first_pass, blocks)
    grad_conv = grad_conv.reshape(TOKENS, C)
    grad_pad = jnp.pad(grad_conv, ((half, half), (0, 0)))

    def second_pass(index):
        start = (index * TOK_DEV).astype(jnp.int32)
        window = lax.dynamic_slice_in_dim(gated_pad, start, TOK_DEV + 2 * half, 0).astype(jnp.float32)
        grad_win = lax.dynamic_slice_in_dim(grad_pad, start, TOK_DEV + 2 * half, 0)
        own = grad_win[half:half + TOK_DEV]
        grad_gated = jnp.zeros((TOK_DEV, C), jnp.float32)
        for offset in range(KERNEL):
            grad_gated = grad_gated + taps[offset] * grad_win[2 * half - offset:2 * half - offset + TOK_DEV]
        tap_terms = jnp.stack([lax.optimization_barrier(jnp.sum(own * window[offset:offset + TOK_DEV], 0)) for offset in range(KERNEL)])
        return (grad_gated, tap_terms)
    grad_gated, tap_parts = lax.map(second_pass, blocks)
    grad_gated = grad_gated.reshape(TOKENS, C)
    scale = 1.0 / math.sqrt(TOKENS)
    d_value = (grad_gated * gate_sig).astype(jnp.bfloat16)
    d_gate = (grad_gated * value_in.astype(jnp.float32) * gate_sig * (1.0 - gate_sig)).astype(jnp.bfloat16)
    d_taps = lax.optimization_barrier(jnp.sum(tap_parts, 0)) * scale
    d_gain = lax.optimization_barrier(jnp.sum(gain_parts, 0)) * scale
    d_shift = lax.optimization_barrier(jnp.sum(shift_parts, 0)) * scale
    return (d_value, d_gate, d_taps, d_gain, d_shift)
```

```python
import functools
import math

import jax
import jax.numpy as jnp
import numpy as np
from jax import lax
from jax.experimental import pallas as pl
from jax.experimental.pallas import tpu as pltpu
from jax.sharding import PartitionSpec as P

EPS = 1e-05
ALIGN = 16
LANES = 128
CHUNK = 256
F32 = jnp.float32
BF16 = jnp.bfloat16


class Plan:
    def __init__(self, rows, kernel, total):
        self.half = kernel // 2
        self.kernel = kernel
        self.rows = rows
        self.edge = -(-(self.half + 1) // ALIGN) * ALIGN
        edge = self.edge
        self.size = rows // 2 + 4 * edge
        size = self.size
        self.freqs = size // 2
        self.wide = rows + 4 * edge
        self.mid = rows + 2 * edge
        self.fwd_out = self.mid // 2
        self.fwd_step = self.wide - size
        self.bwd_out = rows // 2
        self.bwd_step = self.mid - size
        omega = 2.0 * np.pi * (np.arange(self.freqs) + 0.5) / size

        def spectrum(times):
            angle = omega[:, None] * times[None, :]
            return np.concatenate([np.cos(angle), np.sin(angle)], 0)

        def inverse(times):
            angle = times[:, None] * omega[None, :]
            return np.concatenate([np.cos(angle), -np.sin(angle)], 1)

        forward = spectrum(np.arange(size))
        conv = []
        grad = []
        own = []
        for b in range(2):
            start = b * self.fwd_out + edge - self.half - b * self.fwd_step
            conv.append(inverse(np.arange(self.fwd_out) + start))
            start = b * self.bwd_out + edge + self.half - b * self.bwd_step
            grad.append(inverse(np.arange(self.bwd_out) + start))
            start = b * self.bwd_out + edge - b * self.bwd_step
            own.append(spectrum(np.arange(self.bwd_out) + start))
        self.tap_rows = -(-kernel // ALIGN) * ALIGN
        lags = inverse(np.arange(self.tap_rows) - self.half)
        lags[kernel:] = 0.0
        self.mats = np.concatenate([forward] + conv + grad + [lags], 0)
        self.at_conv = size
        self.at_grad = self.at_conv + self.mid
        self.at_lags = self.at_grad + rows
        self.own = np.concatenate(own, 0)
        self.taps = spectrum(np.arange(kernel)) * (2.0 / size)
        self.lag_scale = 2.0 / size / math.sqrt(total)


def dot(a, b):
    return jnp.dot(a, b, preferred_element_type=F32)


def sigmoid(x):
    return 0.5 * jnp.tanh(0.5 * x) + 0.5


def body(
    plan, n, tiles, per, total,
    value_h, gate_h, taps_h, gain_h, shift_h, w_h, go_h, mats_h, own_h, ft_h,
    dv_h, dg_h, dt_o, dgs_o,
    value, gate, taps, gain, shift, w, go, mats, own, ft,
    sig_s, gw, conv, gm, gcw, ts, hs, gs_spec, acc1, acc2,
    st1, st1_in, st2, st2_in, inv_s, colg, cols,
    gs, rs_src, rs_in, ag, dv, dg,
    load_sem, w_sem, out_sem, halo_send, halo_recv, tp_send, tp_recv,
    all_send, all_recv,
):
    sp = lax.axis_index("sp")
    tp = lax.axis_index("tp")
    rows, edge, half2 = plan.rows, plan.edge, 2 * plan.edge
    channels = value.shape[1]
    width = channels * 2
    chunks = channels // CHUNK
    size, freqs, mid = plan.size, plan.freqs, plan.mid
    nxt = lax.rem(sp + 1, n)
    prv = lax.rem(sp + n - 1, n)

    def peer(d):
        return lax.rem(sp + d, n)

    barrier = pltpu.get_barrier_semaphore()

    def greet(d, carry):
        pl.semaphore_signal(
            barrier, 1, device_id=(peer(d), tp), device_id_type=pl.DeviceIdType.MESH
        )
        return carry

    pl.semaphore_signal(
        barrier, 1, device_id=(sp, 1 - tp), device_id_type=pl.DeviceIdType.MESH
    )
    lax.fori_loop(1, n, greet, 0)

    own_go = go.at[pl.ds(edge, rows)]
    pairs = [
        (value_h, value), (gate_h, gate), (taps_h, taps), (ft_h, ft), (own_h, own),
        (mats_h, mats), (go_h, own_go), (gain_h, gain), (shift_h, shift),
    ]
    loads = [
        pltpu.make_async_copy(a, b, load_sem.at[i]) for i, (a, b) in enumerate(pairs)
    ]
    for load in loads:
        load.start()

    def w_copy(c):
        part = pl.ds(pl.multiple_of(c * CHUNK, CHUNK), CHUNK)
        return pltpu.make_async_copy(w_h.at[part], w.at[part], w_sem.at[c])

    for c in range(chunks):
        w_copy(c).start()

    def cut(c):
        return pl.ds(pl.multiple_of(c * CHUNK, CHUNK), CHUNK)

    loads[0].wait()
    loads[1].wait()

    def gate_step(i, carry):
        part = pl.ds(pl.multiple_of(i * ALIGN, ALIGN), ALIGN)
        place = pl.ds(pl.multiple_of(i * ALIGN + half2, ALIGN), ALIGN)
        sig = sigmoid(gate[part].astype(F32))
        sig_s[part] = sig
        gw[place] = (value[part].astype(F32) * sig).astype(BF16)
        return carry

    lax.fori_loop(0, rows // ALIGN, gate_step, 0)
    for load in loads[2:7]:
        load.wait()

    def tap_step(c, carry):
        ts[:, cut(c)] = jnp.dot(
            ft[...], taps[:, cut(c)], precision=lax.Precision.HIGHEST,
            preferred_element_type=F32,
        )
        return carry

    lax.fori_loop(0, chunks, tap_step, 0)

    pl.semaphore_wait(barrier, n)

    def remote(src, dst, send, recv, device):
        return pltpu.make_async_remote_copy(
            src_ref=src, dst_ref=dst, send_sem=send, recv_sem=recv,
            device_id=device, device_id_type=pl.DeviceIdType.MESH,
        )

    halos = [
        remote(gw.at[pl.ds(rows, half2)], gw.at[pl.ds(0, half2)],
               halo_send.at[0], halo_recv.at[0], (nxt, tp)),
        remote(gw.at[pl.ds(half2, half2)], gw.at[pl.ds(rows + half2, half2)],
               halo_send.at[1], halo_recv.at[1], (prv, tp)),
        remote(go.at[pl.ds(rows, edge)], go.at[pl.ds(0, edge)],
               halo_send.at[2], halo_recv.at[2], (nxt, tp)),
        remote(go.at[pl.ds(edge, edge)], go.at[pl.ds(rows + edge, edge)],
               halo_send.at[3], halo_recv.at[3], (prv, tp)),
    ]
    for halo in halos:
        halo.start()

    def mix(a, b):
        return lax.dot_general(a, b, (((1,), (1,)), ((), ())), preferred_element_type=F32)

    def own_step(c, carry):
        for b in range(2):
            hs[pl.ds(b * size, size), cut(c)] = dot(
                own[pl.ds(b * size, size)],
                gw[pl.ds(half2 + b * plan.bwd_out, plan.bwd_out), cut(c)],
            )
        return carry

    lax.fori_loop(0, chunks, own_step, 0)

    def mix_step(c, carry):
        w_copy(c).wait()
        gm[pl.ds(edge, rows), cut(c)] = mix(go[pl.ds(edge, rows)], w[cut(c)])
        return carry

    lax.fori_loop(0, chunks, mix_step, 0)

    halos[0].wait_recv()
    halos[1].wait_recv()

    @pl.when(sp == 0)
    def _():
        gw[pl.ds(0, half2)] = jnp.zeros((half2, channels), BF16)

    @pl.when(sp == n - 1)
    def _():
        gw[pl.ds(rows + half2, half2)] = jnp.zeros((half2, channels), BF16)

    acc1[...] = jnp.zeros_like(acc1)
    acc2[...] = jnp.zeros_like(acc2)

    def fold(x):
        out = x[:, :LANES]
        for k in range(1, x.shape[1] // LANES):
            out = out + x[:, k * LANES : (k + 1) * LANES]
        return out

    def conv_step(c, carry):
        ta = ts[pl.ds(0, freqs), cut(c)]
        tb = ts[pl.ds(freqs, freqs), cut(c)]
        for b in range(2):
            spec = dot(mats[pl.ds(0, size)], gw[pl.ds(b * plan.fwd_step, size), cut(c)])
            re, im = spec[:freqs], spec[freqs:]
            prod = jnp.concatenate([re * ta + im * tb, re * tb - im * ta], 0).astype(BF16)
            out = dot(mats[pl.ds(plan.at_conv + b * plan.fwd_out, plan.fwd_out)], prod)
            place = pl.ds(b * plan.fwd_out, plan.fwd_out)
            conv[place, cut(c)] = out
            acc1[place] += fold(out)
            acc2[place] += fold(out * out)
        return carry

    lax.fori_loop(0, chunks, conv_step, 0)

    first_lanes = lax.broadcasted_iota(jnp.int32, (mid, LANES), 1) < LANES // 2
    st1[...] = jnp.where(
        first_lanes,
        jnp.sum(acc1[...], 1, keepdims=True),
        jnp.sum(acc2[...], 1, keepdims=True),
    )
    swap1 = remote(st1, st1_in, tp_send.at[0], tp_recv.at[0], (sp, 1 - tp))
    swap1.start()

    halos[2].wait_recv()
    halos[3].wait_recv()

    def edge_step(c, carry):
        both = jnp.concatenate([go[pl.ds(0, edge)], go[pl.ds(rows + edge, edge)]], 0)
        out = mix(both, w[cut(c)])
        gm[pl.ds(0, edge), cut(c)] = out[:edge]
        gm[pl.ds(rows + edge, edge), cut(c)] = out[edge:]
        return carry

    lax.fori_loop(0, chunks, edge_step, 0)
    loads[7].wait()
    loads[8].wait()
    colg[...] = jnp.zeros_like(colg)
    cols[...] = jnp.zeros_like(cols)
    swap1.wait_recv()
    lanes = lax.broadcasted_iota(jnp.int32, (ALIGN, LANES), 1) < LANES // 2

    def norm_step(i, carry):
        part = pl.ds(pl.multiple_of(i * ALIGN, ALIGN), ALIGN)
        tot = (st1[part] + st1_in[part]) * (1.0 / width)
        mean = tot[:, :1]
        var = tot[:, LANES // 2 : LANES // 2 + 1] - mean * mean
        inv = lax.rsqrt(var + EPS)
        normed = (conv[part] - mean) * inv
        pre = normed * gain[...] + shift[...]
        sig = sigmoid(pre)
        gp = gm[part] * sig * (1.0 + pre * (1.0 - sig))
        gn = gp * gain[...]
        conv[part] = normed
        gm[part] = gn
        gx = gn * normed
        st2[part] = jnp.where(
            lanes,
            jnp.sum(fold(gn), 1, keepdims=True),
            jnp.sum(fold(gx), 1, keepdims=True),
        )
        inv_s[part] = jnp.broadcast_to(inv, (ALIGN, LANES))

        @pl.when((i >= edge // ALIGN) & (i < (rows + edge) // ALIGN))
        def _():
            gpn = gp * normed
            colg[...] += gpn[:8] + gpn[8:]
            cols[...] += gp[:8] + gp[8:]

        return carry

    lax.fori_loop(0, mid // ALIGN, norm_step, 0)
    swap2 = remote(st2, st2_in, tp_send.at[1], tp_recv.at[1], (sp, 1 - tp))
    swap2.start()

    rg = jnp.sum(colg[...], 0, keepdims=True)
    rsh = jnp.sum(cols[...], 0, keepdims=True)
    groups = channels // LANES
    for k in range(groups):
        gs[sp, pl.ds(k, 1), :] = rg[:, k * LANES : (k + 1) * LANES]
        gs[sp, pl.ds(groups + k, 1), :] = rsh[:, k * LANES : (k + 1) * LANES]

    def send_gs(d, carry):
        remote(gs.at[sp], gs.at[sp], all_send.at[0], all_recv.at[0], (peer(d), tp)).start()
        return carry

    lax.fori_loop(1, n, send_gs, 0)
    swap2.wait_recv()

    def gc_step(i, carry):
        part = pl.ds(pl.multiple_of(i * ALIGN, ALIGN), ALIGN)
        tot = (st2[part] + st2_in[part]) * (1.0 / width)
        m1 = tot[:, :1]
        m2 = tot[:, LANES // 2 : LANES // 2 + 1]
        inv = inv_s[part][:, :1]
        gcw[part] = (inv * (gm[part] - m1 - conv[part] * m2)).astype(BF16)
        return carry

    lax.fori_loop(0, mid // ALIGN, gc_step, 0)

    @pl.when(sp == 0)
    def _():
        gcw[pl.ds(0, edge)] = jnp.zeros((edge, channels), BF16)

    @pl.when(sp == n - 1)
    def _():
        gcw[pl.ds(rows + edge, edge)] = jnp.zeros((edge, channels), BF16)

    if n * per > tiles:
        rs_src[pl.ds(tiles, n * per - tiles)] = jnp.zeros(
            (n * per - tiles, ALIGN, LANES), BF16
        )

    def spec_step(c, carry):
        dr = jnp.zeros((freqs, CHUNK), F32)
        di = jnp.zeros((freqs, CHUNK), F32)
        for b in range(2):
            spec = dot(mats[pl.ds(0, size)], gcw[pl.ds(b * plan.bwd_step, size), cut(c)])
            gs_spec[pl.ds(b * size, size), cut(c)] = spec
            re, im = spec[:freqs], spec[freqs:]
            hr = hs[pl.ds(b * size, freqs), cut(c)]
            hi = hs[pl.ds(b * size + freqs, freqs), cut(c)]
            dr = dr + hr * re + hi * im
            di = di + hr * im - hi * re
        prod = jnp.concatenate([dr, di], 0).astype(BF16)
        out = dot(mats[pl.ds(plan.at_lags, plan.tap_rows)], prod) * plan.lag_scale
        out = out.astype(BF16)
        for r in range(plan.tap_rows // ALIGN):
            for k in range(CHUNK // LANES):
                rs_src[r * groups + c * (CHUNK // LANES) + k] = out[
                    r * ALIGN : (r + 1) * ALIGN, k * LANES : (k + 1) * LANES
                ]
        return carry

    lax.fori_loop(0, chunks, spec_step, 0)

    def send_rs(d, carry):
        to = peer(d)
        remote(rs_src.at[pl.ds(to * per, per)], rs_in.at[sp],
               all_send.at[1], all_recv.at[1], (to, tp)).start()
        return carry

    lax.fori_loop(1, n, send_rs, 0)
    rs_in[sp] = rs_src[pl.ds(sp * per, per)]

    def out_step(c, carry):
        ta = ts[pl.ds(0, freqs), cut(c)]
        tb = ts[pl.ds(freqs, freqs), cut(c)]
        for b in range(2):
            re = gs_spec[pl.ds(b * size, freqs), cut(c)]
            im = gs_spec[pl.ds(b * size + freqs, freqs), cut(c)]
            prod = jnp.concatenate([re * ta - im * tb, -(re * tb + im * ta)], 0).astype(BF16)
            out = dot(mats[pl.ds(plan.at_grad + b * plan.bwd_out, plan.bwd_out)], prod)
            place = pl.ds(b * plan.bwd_out, plan.bwd_out)
            sig = sig_s[place, cut(c)]
            left = out * sig
            dv[place, cut(c)] = left.astype(BF16)
            dg[place, cut(c)] = (
                left * value[place, cut(c)].astype(F32) * (1.0 - sig)
            ).astype(BF16)
        return carry

    lax.fori_loop(0, chunks, out_step, 0)
    outs = [
        pltpu.make_async_copy(dv, dv_h, out_sem.at[0]),
        pltpu.make_async_copy(dg, dg_h, out_sem.at[1]),
    ]
    for out in outs:
        out.start()

    def settle(ref, k):
        part = ref.at[pl.ds(0, n - 1)]
        pltpu.make_async_copy(part, part, all_recv.at[k]).wait()

    def settle_sent(ref, k):
        part = ref.at[pl.ds(0, n - 1)]
        pltpu.make_async_copy(part, part, all_send.at[k]).wait()

    settle(rs_in, 1)
    zero = jnp.zeros((per, ALIGN, LANES), F32)
    summed = lax.fori_loop(0, n, lambda i, t: t + rs_in[i].astype(F32), zero)
    ag[sp] = summed.astype(BF16)

    def send_ag(d, carry):
        remote(ag.at[sp], ag.at[sp], all_send.at[2], all_recv.at[2], (peer(d), tp)).start()
        return carry

    lax.fori_loop(1, n, send_ag, 0)

    settle(gs, 0)
    small = lax.fori_loop(
        0, n, lambda i, t: t + gs[i], jnp.zeros(gs.shape[1:], F32)
    )
    dgs_o[...] = small * (1.0 / math.sqrt(total))

    for halo in halos:
        halo.wait_send()
    swap1.wait_send()
    swap2.wait_send()
    settle_sent(gs, 0)
    settle_sent(rs_in, 1)
    settle(ag, 2)
    for t in range(tiles):
        r, k = t // groups, t % groups
        count = min(ALIGN, plan.kernel - r * ALIGN)
        dt_o[pl.ds(r * ALIGN, count), pl.ds(k * LANES, LANES)] = ag[t // per, t % per].astype(F32)[
            :count
        ]
    settle_sent(ag, 2)
    for out in outs:
        out.wait()


def shards(n, value_in, gate_in, taps, gain, shift, w_out, grad_out):
    rows, channels = value_in.shape
    kernel = taps.shape[0]
    total = rows * n
    plan = Plan(rows, kernel, total)
    groups = channels // LANES
    tiles = plan.tap_rows // ALIGN * groups
    per = -(-tiles // n)
    model = grad_out.shape[1]
    mats = jnp.asarray(plan.mats, BF16)
    own = jnp.asarray(plan.own, BF16)
    ft = jnp.asarray(plan.taps, F32)
    hbm = pl.BlockSpec(memory_space=pl.ANY)
    vmem = pl.BlockSpec(memory_space=pltpu.VMEM)
    size, mid = plan.size, plan.mid
    chunks = channels // CHUNK
    dma = pltpu.SemaphoreType.DMA
    d_value, d_gate, d_taps, d_small = pl.pallas_call(
        functools.partial(body, plan, n, tiles, per, total),
        out_shape=(
            jax.ShapeDtypeStruct((rows, channels), BF16),
            jax.ShapeDtypeStruct((rows, channels), BF16),
            jax.ShapeDtypeStruct((kernel, channels), F32),
            jax.ShapeDtypeStruct((2 * groups, LANES), F32),
        ),
        in_specs=[hbm] * 10,
        out_specs=(hbm, hbm, vmem, vmem),
        scratch_shapes=[
            pltpu.VMEM((rows, channels), BF16),
            pltpu.VMEM((rows, channels), BF16),
            pltpu.VMEM((kernel, channels), F32),
            pltpu.VMEM((1, channels), F32),
            pltpu.VMEM((1, channels), F32),
            pltpu.VMEM((channels, model), BF16),
            pltpu.VMEM((mid, model), BF16),
            pltpu.VMEM(plan.mats.shape, BF16),
            pltpu.VMEM(plan.own.shape, BF16),
            pltpu.VMEM(plan.taps.shape, F32),
            pltpu.VMEM((rows, channels), F32),
            pltpu.VMEM((plan.wide, channels), BF16),
            pltpu.VMEM((mid, channels), F32),
            pltpu.VMEM((mid, channels), F32),
            pltpu.VMEM((mid, channels), BF16),
            pltpu.VMEM((size, channels), F32),
            pltpu.VMEM((2 * size, channels), F32),
            pltpu.VMEM((2 * size, channels), F32),
            pltpu.VMEM((mid, LANES), F32),
            pltpu.VMEM((mid, LANES), F32),
            pltpu.VMEM((mid, LANES), F32),
            pltpu.VMEM((mid, LANES), F32),
            pltpu.VMEM((mid, LANES), F32),
            pltpu.VMEM((mid, LANES), F32),
            pltpu.VMEM((mid, LANES), F32),
            pltpu.VMEM((8, channels), F32),
            pltpu.VMEM((8, channels), F32),
            pltpu.VMEM((n, 2 * groups, LANES), F32),
            pltpu.VMEM((n * per, ALIGN, LANES), BF16),
            pltpu.VMEM((n, per, ALIGN, LANES), BF16),
            pltpu.VMEM((n, per, ALIGN, LANES), BF16),
            pltpu.VMEM((rows, channels), BF16),
            pltpu.VMEM((rows, channels), BF16),
            dma((9,)), dma((chunks,)), dma((2,)), dma((4,)), dma((4,)),
            dma((2,)), dma((2,)), dma((3,)), dma((3,)),
        ],
        compiler_params=pltpu.CompilerParams(
            collective_id=0, has_side_effects=True, vmem_limit_bytes=48 * 1024 * 1024
        ),
    )(
        value_in, gate_in, taps, gain.reshape(1, -1), shift.reshape(1, -1), w_out,
        grad_out, mats, own, ft,
    )
    flat = d_small.reshape(2, channels)
    return (d_value, d_gate, d_taps, flat[0], flat[1])


def solution(mesh):
    return jax.shard_map(
        functools.partial(shards, mesh.shape["sp"]),
        mesh=mesh,
        in_specs=(
            P("sp", "tp"),
            P("sp", "tp"),
            P(None, "tp"),
            P("tp"),
            P("tp"),
            P("tp", None),
            P("sp", None),
        ),
        out_specs=(P("sp", "tp"), P("sp", "tp"), P(None, "tp"), P("tp"), P("tp")),
        check_vma=False,
    )
```

```python
import functools
import math

import jax
import jax.numpy as jnp
import numpy as np
from jax import lax
from jax.experimental import pallas as pl
from jax.experimental.pallas import tpu as pltpu
from jax.sharding import PartitionSpec as P

EPS = 1e-05
ALIGN = 16
LANES = 128
CHUNK = 256
F32 = jnp.float32
BF16 = jnp.bfloat16


class Plan:
    def __init__(self, rows, kernel, total):
        self.half = kernel // 2
        self.kernel = kernel
        self.rows = rows
        self.edge = -(-(self.half + 1) // ALIGN) * ALIGN
        edge = self.edge
        self.size = rows // 2 + 4 * edge
        size = self.size
        self.freqs = size // 2
        self.wide = rows + 4 * edge
        self.mid = rows + 2 * edge
        self.fwd_out = self.mid // 2
        self.fwd_step = self.wide - size
        self.bwd_out = rows // 2
        self.bwd_step = self.mid - size
        omega = 2.0 * np.pi * (np.arange(self.freqs) + 0.5) / size

        def spectrum(times):
            angle = omega[:, None] * times[None, :]
            return np.concatenate([np.cos(angle), np.sin(angle)], 0)

        def inverse(times):
            angle = times[:, None] * omega[None, :]
            return np.concatenate([np.cos(angle), -np.sin(angle)], 1)

        forward = spectrum(np.arange(size))
        conv = []
        grad = []
        own = []
        for b in range(2):
            start = b * self.fwd_out + edge - self.half - b * self.fwd_step
            conv.append(inverse(np.arange(self.fwd_out) + start))
            start = b * self.bwd_out + edge + self.half - b * self.bwd_step
            grad.append(inverse(np.arange(self.bwd_out) + start))
            start = b * self.bwd_out + edge - b * self.bwd_step
            own.append(spectrum(np.arange(self.bwd_out) + start))
        self.tap_rows = -(-kernel // ALIGN) * ALIGN
        lags = inverse(np.arange(self.tap_rows) - self.half)
        lags[kernel:] = 0.0
        self.mats = np.concatenate([forward] + conv + grad + [lags], 0)
        self.at_conv = size
        self.at_grad = self.at_conv + self.mid
        self.at_lags = self.at_grad + rows
        self.own = np.concatenate(own, 0)
        self.taps = spectrum(np.arange(kernel)) * (2.0 / size)
        self.lag_scale = 2.0 / size / math.sqrt(total)


def dot(a, b):
    return jnp.dot(a, b, preferred_element_type=F32)


def sigmoid(x):
    return 0.5 * jnp.tanh(0.5 * x) + 0.5


def body(
    plan, n, tiles, per, total,
    value_h, gate_h, taps_h, gain_h, shift_h, w_h, go_h, mats_h, own_h, ft_h,
    dv, dg, dt_o, dgs_o,
    value, gate, taps, gain, shift, w, go, mats, own, ft,
    sig_s, gw, conv, gm, gcw, ts, hs, gs_spec, acc1, acc2,
    st1, st1_in, st2, st2_in, inv_s, colg, cols,
    gs, rs_src, rs_in, ag,
    load_sem, w_sem, halo_send, halo_recv, tp_send, tp_recv,
    all_send, all_recv,
):
    sp = lax.axis_index("sp")
    tp = lax.axis_index("tp")
    rows, edge, half2 = plan.rows, plan.edge, 2 * plan.edge
    channels = value.shape[1]
    width = channels * 2
    chunks = channels // CHUNK
    size, freqs, mid = plan.size, plan.freqs, plan.mid
    nxt = lax.rem(sp + 1, n)
    prv = lax.rem(sp + n - 1, n)

    def peer(d):
        return lax.rem(sp + d, n)

    barrier = pltpu.get_barrier_semaphore()

    def greet(d, carry):
        pl.semaphore_signal(
            barrier, 1, device_id=(peer(d), tp), device_id_type=pl.DeviceIdType.MESH
        )
        return carry

    pl.semaphore_signal(
        barrier, 1, device_id=(sp, 1 - tp), device_id_type=pl.DeviceIdType.MESH
    )
    lax.fori_loop(1, n, greet, 0)

    own_go = go.at[pl.ds(edge, rows)]
    pairs = [
        (value_h, value), (gate_h, gate), (taps_h, taps), (ft_h, ft), (own_h, own),
        (mats_h, mats), (go_h, own_go), (gain_h, gain), (shift_h, shift),
    ]
    loads = [
        pltpu.make_async_copy(a, b, load_sem.at[i]) for i, (a, b) in enumerate(pairs)
    ]
    for load in loads:
        load.start()

    def w_copy(c):
        part = pl.ds(pl.multiple_of(c * CHUNK, CHUNK), CHUNK)
        return pltpu.make_async_copy(w_h.at[part], w.at[part], w_sem.at[c])

    for c in range(chunks):
        w_copy(c).start()

    def cut(c):
        return pl.ds(pl.multiple_of(c * CHUNK, CHUNK), CHUNK)

    loads[0].wait()
    loads[1].wait()

    def gate_step(i, carry):
        part = pl.ds(pl.multiple_of(i * ALIGN, ALIGN), ALIGN)
        place = pl.ds(pl.multiple_of(i * ALIGN + half2, ALIGN), ALIGN)
        sig = sigmoid(gate[part].astype(F32))
        sig_s[part] = sig
        gw[place] = (value[part].astype(F32) * sig).astype(BF16)
        return carry

    lax.fori_loop(0, rows // ALIGN, gate_step, 0)
    for load in loads[2:7]:
        load.wait()

    def tap_step(c, carry):
        ts[:, cut(c)] = jnp.dot(
            ft[...], taps[:, cut(c)], precision=lax.Precision.HIGHEST,
            preferred_element_type=F32,
        )
        return carry

    lax.fori_loop(0, chunks, tap_step, 0)

    pl.semaphore_wait(barrier, n)

    def remote(src, dst, send, recv, device):
        return pltpu.make_async_remote_copy(
            src_ref=src, dst_ref=dst, send_sem=send, recv_sem=recv,
            device_id=device, device_id_type=pl.DeviceIdType.MESH,
        )

    halos = [
        remote(gw.at[pl.ds(rows, half2)], gw.at[pl.ds(0, half2)],
               halo_send.at[0], halo_recv.at[0], (nxt, tp)),
        remote(gw.at[pl.ds(half2, half2)], gw.at[pl.ds(rows + half2, half2)],
               halo_send.at[1], halo_recv.at[1], (prv, tp)),
        remote(go.at[pl.ds(rows, edge)], go.at[pl.ds(0, edge)],
               halo_send.at[2], halo_recv.at[2], (nxt, tp)),
        remote(go.at[pl.ds(edge, edge)], go.at[pl.ds(rows + edge, edge)],
               halo_send.at[3], halo_recv.at[3], (prv, tp)),
    ]
    for halo in halos:
        halo.start()

    def mix(a, b):
        return lax.dot_general(a, b, (((1,), (1,)), ((), ())), preferred_element_type=F32)

    def own_step(c, carry):
        for b in range(2):
            hs[pl.ds(b * size, size), cut(c)] = dot(
                own[pl.ds(b * size, size)],
                gw[pl.ds(half2 + b * plan.bwd_out, plan.bwd_out), cut(c)],
            )
        return carry

    lax.fori_loop(0, chunks, own_step, 0)

    def mix_step(c, carry):
        w_copy(c).wait()
        gm[pl.ds(edge, rows), cut(c)] = mix(go[pl.ds(edge, rows)], w[cut(c)])
        return carry

    lax.fori_loop(0, chunks, mix_step, 0)

    halos[0].wait_recv()
    halos[1].wait_recv()

    @pl.when(sp == 0)
    def _():
        gw[pl.ds(0, half2)] = jnp.zeros((half2, channels), BF16)

    @pl.when(sp == n - 1)
    def _():
        gw[pl.ds(rows + half2, half2)] = jnp.zeros((half2, channels), BF16)

    acc1[...] = jnp.zeros_like(acc1)
    acc2[...] = jnp.zeros_like(acc2)

    def fold(x):
        out = x[:, :LANES]
        for k in range(1, x.shape[1] // LANES):
            out = out + x[:, k * LANES : (k + 1) * LANES]
        return out

    def conv_step(c, carry):
        ta = ts[pl.ds(0, freqs), cut(c)]
        tb = ts[pl.ds(freqs, freqs), cut(c)]
        for b in range(2):
            spec = dot(mats[pl.ds(0, size)], gw[pl.ds(b * plan.fwd_step, size), cut(c)])
            re, im = spec[:freqs], spec[freqs:]
            prod = jnp.concatenate([re * ta + im * tb, re * tb - im * ta], 0).astype(BF16)
            out = dot(mats[pl.ds(plan.at_conv + b * plan.fwd_out, plan.fwd_out)], prod)
            place = pl.ds(b * plan.fwd_out, plan.fwd_out)
            conv[place, cut(c)] = out
            acc1[place] += fold(out)
            acc2[place] += fold(out * out)
        return carry

    lax.fori_loop(0, chunks, conv_step, 0)

    first_lanes = lax.broadcasted_iota(jnp.int32, (mid, LANES), 1) < LANES // 2
    st1[...] = jnp.where(
        first_lanes,
        jnp.sum(acc1[...], 1, keepdims=True),
        jnp.sum(acc2[...], 1, keepdims=True),
    )
    swap1 = remote(st1, st1_in, tp_send.at[0], tp_recv.at[0], (sp, 1 - tp))
    swap1.start()

    halos[2].wait_recv()
    halos[3].wait_recv()

    def edge_step(c, carry):
        both = jnp.concatenate([go[pl.ds(0, edge)], go[pl.ds(rows + edge, edge)]], 0)
        out = mix(both, w[cut(c)])
        gm[pl.ds(0, edge), cut(c)] = out[:edge]
        gm[pl.ds(rows + edge, edge), cut(c)] = out[edge:]
        return carry

    lax.fori_loop(0, chunks, edge_step, 0)
    loads[7].wait()
    loads[8].wait()
    colg[...] = jnp.zeros_like(colg)
    cols[...] = jnp.zeros_like(cols)
    swap1.wait_recv()
    lanes = lax.broadcasted_iota(jnp.int32, (ALIGN, LANES), 1) < LANES // 2

    def norm_step(i, carry):
        part = pl.ds(pl.multiple_of(i * ALIGN, ALIGN), ALIGN)
        tot = (st1[part] + st1_in[part]) * (1.0 / width)
        mean = tot[:, :1]
        var = tot[:, LANES // 2 : LANES // 2 + 1] - mean * mean
        inv = lax.rsqrt(var + EPS)
        normed = (conv[part] - mean) * inv
        pre = normed * gain[...] + shift[...]
        sig = sigmoid(pre)
        gp = gm[part] * sig * (1.0 + pre * (1.0 - sig))
        gn = gp * gain[...]
        conv[part] = normed
        gm[part] = gn
        gx = gn * normed
        st2[part] = jnp.where(
            lanes,
            jnp.sum(fold(gn), 1, keepdims=True),
            jnp.sum(fold(gx), 1, keepdims=True),
        )
        inv_s[part] = jnp.broadcast_to(inv, (ALIGN, LANES))

        @pl.when((i >= edge // ALIGN) & (i < (rows + edge) // ALIGN))
        def _():
            gpn = gp * normed
            colg[...] += gpn[:8] + gpn[8:]
            cols[...] += gp[:8] + gp[8:]

        return carry

    lax.fori_loop(0, mid // ALIGN, norm_step, 0)
    swap2 = remote(st2, st2_in, tp_send.at[1], tp_recv.at[1], (sp, 1 - tp))
    swap2.start()

    rg = jnp.sum(colg[...], 0, keepdims=True)
    rsh = jnp.sum(cols[...], 0, keepdims=True)
    groups = channels // LANES
    for k in range(groups):
        gs[sp, pl.ds(k, 1), :] = rg[:, k * LANES : (k + 1) * LANES]
        gs[sp, pl.ds(groups + k, 1), :] = rsh[:, k * LANES : (k + 1) * LANES]

    def send_gs(d, carry):
        remote(gs.at[sp], gs.at[sp], all_send.at[0], all_recv.at[0], (peer(d), tp)).start()
        return carry

    lax.fori_loop(1, n, send_gs, 0)
    swap2.wait_recv()

    def gc_step(i, carry):
        part = pl.ds(pl.multiple_of(i * ALIGN, ALIGN), ALIGN)
        tot = (st2[part] + st2_in[part]) * (1.0 / width)
        m1 = tot[:, :1]
        m2 = tot[:, LANES // 2 : LANES // 2 + 1]
        inv = inv_s[part][:, :1]
        gcw[part] = (inv * (gm[part] - m1 - conv[part] * m2)).astype(BF16)
        return carry

    lax.fori_loop(0, mid // ALIGN, gc_step, 0)

    @pl.when(sp == 0)
    def _():
        gcw[pl.ds(0, edge)] = jnp.zeros((edge, channels), BF16)

    @pl.when(sp == n - 1)
    def _():
        gcw[pl.ds(rows + edge, edge)] = jnp.zeros((edge, channels), BF16)

    if n * per > tiles:
        rs_src[pl.ds(tiles, n * per - tiles)] = jnp.zeros(
            (n * per - tiles, ALIGN, LANES), BF16
        )

    def spec_step(c, carry):
        dr = jnp.zeros((freqs, CHUNK), F32)
        di = jnp.zeros((freqs, CHUNK), F32)
        for b in range(2):
            spec = dot(mats[pl.ds(0, size)], gcw[pl.ds(b * plan.bwd_step, size), cut(c)])
            gs_spec[pl.ds(b * size, size), cut(c)] = spec
            re, im = spec[:freqs], spec[freqs:]
            hr = hs[pl.ds(b * size, freqs), cut(c)]
            hi = hs[pl.ds(b * size + freqs, freqs), cut(c)]
            dr = dr + hr * re + hi * im
            di = di + hr * im - hi * re
        prod = jnp.concatenate([dr, di], 0).astype(BF16)
        out = dot(mats[pl.ds(plan.at_lags, plan.tap_rows)], prod) * plan.lag_scale
        out = out.astype(BF16)
        for r in range(plan.tap_rows // ALIGN):
            for k in range(CHUNK // LANES):
                rs_src[r * groups + c * (CHUNK // LANES) + k] = out[
                    r * ALIGN : (r + 1) * ALIGN, k * LANES : (k + 1) * LANES
                ]
        return carry

    lax.fori_loop(0, chunks, spec_step, 0)

    def send_rs(d, carry):
        to = peer(d)
        remote(rs_src.at[pl.ds(to * per, per)], rs_in.at[sp],
               all_send.at[1], all_recv.at[1], (to, tp)).start()
        return carry

    lax.fori_loop(1, n, send_rs, 0)
    rs_in[sp] = rs_src[pl.ds(sp * per, per)]

    def out_step(c, carry):
        ta = ts[pl.ds(0, freqs), cut(c)]
        tb = ts[pl.ds(freqs, freqs), cut(c)]
        for b in range(2):
            re = gs_spec[pl.ds(b * size, freqs), cut(c)]
            im = gs_spec[pl.ds(b * size + freqs, freqs), cut(c)]
            prod = jnp.concatenate([re * ta - im * tb, -(re * tb + im * ta)], 0).astype(BF16)
            out = dot(mats[pl.ds(plan.at_grad + b * plan.bwd_out, plan.bwd_out)], prod)
            place = pl.ds(b * plan.bwd_out, plan.bwd_out)
            sig = sig_s[place, cut(c)]
            left = out * sig
            dv[place, cut(c)] = left.astype(BF16)
            dg[place, cut(c)] = (
                left * value[place, cut(c)].astype(F32) * (1.0 - sig)
            ).astype(BF16)
        return carry

    lax.fori_loop(0, chunks, out_step, 0)
    def settle(ref, k):
        part = ref.at[pl.ds(0, n - 1)]
        pltpu.make_async_copy(part, part, all_recv.at[k]).wait()

    def settle_sent(ref, k):
        part = ref.at[pl.ds(0, n - 1)]
        pltpu.make_async_copy(part, part, all_send.at[k]).wait()

    settle(rs_in, 1)
    zero = jnp.zeros((per, ALIGN, LANES), F32)
    summed = lax.fori_loop(0, n, lambda i, t: t + rs_in[i].astype(F32), zero)
    ag[sp] = summed.astype(BF16)

    def send_ag(d, carry):
        remote(ag.at[sp], ag.at[sp], all_send.at[2], all_recv.at[2], (peer(d), tp)).start()
        return carry

    lax.fori_loop(1, n, send_ag, 0)

    settle(gs, 0)
    small = lax.fori_loop(
        0, n, lambda i, t: t + gs[i], jnp.zeros(gs.shape[1:], F32)
    )
    dgs_o[...] = small * (1.0 / math.sqrt(total))

    for halo in halos:
        halo.wait_send()
    swap1.wait_send()
    swap2.wait_send()
    settle_sent(gs, 0)
    settle_sent(rs_in, 1)
    settle(ag, 2)
    for t in range(tiles):
        r, k = t // groups, t % groups
        count = min(ALIGN, plan.kernel - r * ALIGN)
        dt_o[pl.ds(r * ALIGN, count), pl.ds(k * LANES, LANES)] = ag[t // per, t % per].astype(F32)[
            :count
        ]
    settle_sent(ag, 2)


def store(parts, *refs):
    sources, targets, sem = refs[:parts], refs[parts:-1], refs[-1]
    groups = sources[-1].shape[0] // 2
    views = list(sources[:-1]) + [
        sources[-1].at[pl.ds(0, groups)], sources[-1].at[pl.ds(groups, groups)]
    ]
    copies = [
        pltpu.make_async_copy(a, b, sem.at[i]) for i, (a, b) in enumerate(zip(views, targets))
    ]
    for copy in copies:
        copy.start()
    for copy in copies:
        copy.wait()


def shards(n, value_in, gate_in, taps, gain, shift, w_out, grad_out):
    rows, channels = value_in.shape
    kernel = taps.shape[0]
    total = rows * n
    plan = Plan(rows, kernel, total)
    groups = channels // LANES
    tiles = plan.tap_rows // ALIGN * groups
    per = -(-tiles // n)
    model = grad_out.shape[1]
    mats = jnp.asarray(plan.mats, BF16)
    own = jnp.asarray(plan.own, BF16)
    ft = jnp.asarray(plan.taps, F32)
    hbm = pl.BlockSpec(memory_space=pltpu.HBM)
    vmem = pl.BlockSpec(memory_space=pltpu.VMEM)
    size, mid = plan.size, plan.mid
    chunks = channels // CHUNK
    dma = pltpu.SemaphoreType.DMA
    results = pl.pallas_call(
        functools.partial(body, plan, n, tiles, per, total),
        out_shape=(
            jax.ShapeDtypeStruct((rows, channels), BF16),
            jax.ShapeDtypeStruct((rows, channels), BF16),
            jax.ShapeDtypeStruct((kernel, channels), F32),
            jax.ShapeDtypeStruct((2 * groups, LANES), F32),
        ),
        in_specs=[hbm] * 10,
        out_specs=(vmem,) * 4,
        scratch_shapes=[
            pltpu.VMEM((rows, channels), BF16),
            pltpu.VMEM((rows, channels), BF16),
            pltpu.VMEM((kernel, channels), F32),
            pltpu.VMEM((1, channels), F32),
            pltpu.VMEM((1, channels), F32),
            pltpu.VMEM((channels, model), BF16),
            pltpu.VMEM((mid, model), BF16),
            pltpu.VMEM(plan.mats.shape, BF16),
            pltpu.VMEM(plan.own.shape, BF16),
            pltpu.VMEM(plan.taps.shape, F32),
            pltpu.VMEM((rows, channels), F32),
            pltpu.VMEM((plan.wide, channels), BF16),
            pltpu.VMEM((mid, channels), F32),
            pltpu.VMEM((mid, channels), F32),
            pltpu.VMEM((mid, channels), BF16),
            pltpu.VMEM((size, channels), F32),
            pltpu.VMEM((2 * size, channels), F32),
            pltpu.VMEM((2 * size, channels), F32),
            pltpu.VMEM((mid, LANES), F32),
            pltpu.VMEM((mid, LANES), F32),
            pltpu.VMEM((mid, LANES), F32),
            pltpu.VMEM((mid, LANES), F32),
            pltpu.VMEM((mid, LANES), F32),
            pltpu.VMEM((mid, LANES), F32),
            pltpu.VMEM((mid, LANES), F32),
            pltpu.VMEM((8, channels), F32),
            pltpu.VMEM((8, channels), F32),
            pltpu.VMEM((n, 2 * groups, LANES), F32),
            pltpu.VMEM((n * per, ALIGN, LANES), BF16),
            pltpu.VMEM((n, per, ALIGN, LANES), BF16),
            pltpu.VMEM((n, per, ALIGN, LANES), BF16),
            dma((9,)), dma((chunks,)), dma((4,)), dma((4,)),
            dma((2,)), dma((2,)), dma((3,)), dma((3,)),
        ],
        compiler_params=pltpu.CompilerParams(
            collective_id=0, has_side_effects=True, vmem_limit_bytes=48 * 1024 * 1024
        ),
    )(
        value_in, gate_in, taps, gain.reshape(1, -1), shift.reshape(1, -1), w_out,
        grad_out, mats, own, ft,
    )
    d_value, d_gate, d_taps, d_gain, d_shift = pl.pallas_call(
        functools.partial(store, 4),
        out_shape=(
            jax.ShapeDtypeStruct((rows, channels), BF16),
            jax.ShapeDtypeStruct((rows, channels), BF16),
            jax.ShapeDtypeStruct((kernel, channels), F32),
            jax.ShapeDtypeStruct((groups, LANES), F32),
            jax.ShapeDtypeStruct((groups, LANES), F32),
        ),
        in_specs=[vmem] * 4,
        out_specs=(hbm,) * 5,
        scratch_shapes=[dma((5,))],
    )(*results)
    return (d_value, d_gate, d_taps, d_gain.reshape(-1), d_shift.reshape(-1))


def solution(mesh):
    return jax.shard_map(
        functools.partial(shards, mesh.shape["sp"]),
        mesh=mesh,
        in_specs=(
            P("sp", "tp"),
            P("sp", "tp"),
            P(None, "tp"),
            P("tp"),
            P("tp"),
            P("tp", None),
            P("sp", None),
        ),
        out_specs=(P("sp", "tp"), P("sp", "tp"), P(None, "tp"), P("tp"), P("tp")),
        check_vma=False,
    )
```

```python
import functools
import math

import jax
import jax.numpy as jnp
import numpy as np
from jax import lax
from jax.experimental import pallas as pl
from jax.experimental.pallas import tpu as pltpu
from jax.sharding import PartitionSpec as P

EPS = 1e-05
ALIGN = 16
LANES = 128
CHUNK = 256
VMEM_GRANT = 62 * 1024 * 1024
F32 = jnp.float32
BF16 = jnp.bfloat16


class Plan:
    def __init__(self, rows, kernel, total):
        self.half = kernel // 2
        self.kernel = kernel
        self.rows = rows
        self.edge = -(-(self.half + 1) // ALIGN) * ALIGN
        edge = self.edge
        self.size = rows // 2 + 4 * edge
        size = self.size
        self.freqs = size // 2
        self.wide = rows + 4 * edge
        self.mid = rows + 2 * edge
        self.fwd_out = self.mid // 2
        self.fwd_step = self.wide - size
        self.bwd_out = rows // 2
        self.bwd_step = self.mid - size
        omega = 2.0 * np.pi * (np.arange(self.freqs) + 0.5) / size

        def spectrum(times):
            angle = omega[:, None] * times[None, :]
            return np.concatenate([np.cos(angle), np.sin(angle)], 0)

        def inverse(times):
            angle = times[:, None] * omega[None, :]
            return np.concatenate([np.cos(angle), -np.sin(angle)], 1)

        forward = spectrum(np.arange(size))
        conv = []
        grad = []
        own = []
        for b in range(2):
            start = b * self.fwd_out + edge - self.half - b * self.fwd_step
            conv.append(inverse(np.arange(self.fwd_out) + start))
            start = b * self.bwd_out + edge + self.half - b * self.bwd_step
            grad.append(inverse(np.arange(self.bwd_out) + start))
            start = b * self.bwd_out + edge - b * self.bwd_step
            own.append(spectrum(np.arange(self.bwd_out) + start))
        self.tap_rows = -(-kernel // ALIGN) * ALIGN
        lags = inverse(np.arange(self.tap_rows) - self.half)
        lags[kernel:] = 0.0
        self.mats = np.concatenate([forward] + conv + grad + [lags], 0)
        self.at_conv = size
        self.at_grad = self.at_conv + self.mid
        self.at_lags = self.at_grad + rows
        self.own = np.concatenate(own, 0)
        self.taps = spectrum(np.arange(kernel)) * (2.0 / size)
        self.lag_scale = 2.0 / size / math.sqrt(total)


def dot(a, b):
    return jnp.dot(a, b, preferred_element_type=F32)


def sigmoid(x):
    return 0.5 * jnp.tanh(0.5 * x) + 0.5


def body(
    plan, n, tiles, per, total,
    value_h, gate_h, taps_h, gain_h, shift_h, w_h, go_h, mats_h, own_h, ft_h,
    dv_h, dg_h, dt_o, dgs_o,
    value, gate, taps, gain, shift, w, go, mats, own, ft,
    sig_s, gw, conv, gm, gcw, ts, hs, gs_spec, acc1, acc2,
    st1, st1_in, st2, st2_in, inv_s, colg, cols,
    gs, rs_src, rs_in, ag, dv, dg,
    load_sem, w_sem, out_sem, halo_send, halo_recv, tp_send, tp_recv,
    all_send, all_recv,
):
    sp = lax.axis_index("sp")
    tp = lax.axis_index("tp")
    rows, edge, half2 = plan.rows, plan.edge, 2 * plan.edge
    channels = value.shape[1]
    width = channels * 2
    chunks = channels // CHUNK
    size, freqs, mid = plan.size, plan.freqs, plan.mid
    nxt = lax.rem(sp + 1, n)
    prv = lax.rem(sp + n - 1, n)

    def peer(d):
        return lax.rem(sp + d, n)

    barrier = pltpu.get_barrier_semaphore()

    def greet(d, carry):
        pl.semaphore_signal(
            barrier, 1, device_id=(peer(d), tp), device_id_type=pl.DeviceIdType.MESH
        )
        return carry

    pl.semaphore_signal(
        barrier, 1, device_id=(sp, 1 - tp), device_id_type=pl.DeviceIdType.MESH
    )
    lax.fori_loop(1, n, greet, 0)

    own_go = go.at[pl.ds(edge, rows)]
    pairs = [
        (value_h, value), (gate_h, gate), (taps_h, taps), (ft_h, ft), (own_h, own),
        (mats_h, mats), (go_h, own_go), (gain_h, gain), (shift_h, shift),
    ]
    loads = [
        pltpu.make_async_copy(a, b, load_sem.at[i]) for i, (a, b) in enumerate(pairs)
    ]
    for load in loads:
        load.start()

    def w_copy(c):
        part = pl.ds(pl.multiple_of(c * CHUNK, CHUNK), CHUNK)
        return pltpu.make_async_copy(w_h.at[part], w.at[part], w_sem.at[c])

    for c in range(chunks):
        w_copy(c).start()

    def cut(c):
        return pl.ds(pl.multiple_of(c * CHUNK, CHUNK), CHUNK)

    loads[0].wait()
    loads[1].wait()

    def gate_step(i, carry):
        part = pl.ds(pl.multiple_of(i * ALIGN, ALIGN), ALIGN)
        place = pl.ds(pl.multiple_of(i * ALIGN + half2, ALIGN), ALIGN)
        sig = sigmoid(gate[part].astype(F32))
        sig_s[part] = sig
        gw[place] = (value[part].astype(F32) * sig).astype(BF16)
        return carry

    lax.fori_loop(0, rows // ALIGN, gate_step, 0)
    for load in loads[2:7]:
        load.wait()

    def tap_step(c, carry):
        ts[:, cut(c)] = jnp.dot(
            ft[...], taps[:, cut(c)], precision=lax.Precision.HIGHEST,
            preferred_element_type=F32,
        )
        return carry

    lax.fori_loop(0, chunks, tap_step, 0)

    pl.semaphore_wait(barrier, n)

    def remote(src, dst, send, recv, device):
        return pltpu.make_async_remote_copy(
            src_ref=src, dst_ref=dst, send_sem=send, recv_sem=recv,
            device_id=device, device_id_type=pl.DeviceIdType.MESH,
        )

    halos = [
        remote(gw.at[pl.ds(rows, half2)], gw.at[pl.ds(0, half2)],
               halo_send.at[0], halo_recv.at[0], (nxt, tp)),
        remote(gw.at[pl.ds(half2, half2)], gw.at[pl.ds(rows + half2, half2)],
               halo_send.at[1], halo_recv.at[1], (prv, tp)),
        remote(go.at[pl.ds(rows, edge)], go.at[pl.ds(0, edge)],
               halo_send.at[2], halo_recv.at[2], (nxt, tp)),
        remote(go.at[pl.ds(edge, edge)], go.at[pl.ds(rows + edge, edge)],
               halo_send.at[3], halo_recv.at[3], (prv, tp)),
    ]
    for halo in halos:
        halo.start()

    def mix(a, b):
        return lax.dot_general(a, b, (((1,), (1,)), ((), ())), preferred_element_type=F32)

    def own_step(c, carry):
        for b in range(2):
            hs[pl.ds(b * size, size), cut(c)] = dot(
                own[pl.ds(b * size, size)],
                gw[pl.ds(half2 + b * plan.bwd_out, plan.bwd_out), cut(c)],
            )
        return carry

    lax.fori_loop(0, chunks, own_step, 0)

    def mix_step(c, carry):
        w_copy(c).wait()
        gm[pl.ds(edge, rows), cut(c)] = mix(go[pl.ds(edge, rows)], w[cut(c)])
        return carry

    lax.fori_loop(0, chunks, mix_step, 0)

    halos[0].wait_recv()
    halos[1].wait_recv()

    @pl.when(sp == 0)
    def _():
        gw[pl.ds(0, half2)] = jnp.zeros((half2, channels), BF16)

    @pl.when(sp == n - 1)
    def _():
        gw[pl.ds(rows + half2, half2)] = jnp.zeros((half2, channels), BF16)

    acc1[...] = jnp.zeros_like(acc1)
    acc2[...] = jnp.zeros_like(acc2)

    def fold(x):
        out = x[:, :LANES]
        for k in range(1, x.shape[1] // LANES):
            out = out + x[:, k * LANES : (k + 1) * LANES]
        return out

    def conv_step(c, carry):
        ta = ts[pl.ds(0, freqs), cut(c)]
        tb = ts[pl.ds(freqs, freqs), cut(c)]
        for b in range(2):
            spec = dot(mats[pl.ds(0, size)], gw[pl.ds(b * plan.fwd_step, size), cut(c)])
            re, im = spec[:freqs], spec[freqs:]
            prod = jnp.concatenate([re * ta + im * tb, re * tb - im * ta], 0).astype(BF16)
            out = dot(mats[pl.ds(plan.at_conv + b * plan.fwd_out, plan.fwd_out)], prod)
            place = pl.ds(b * plan.fwd_out, plan.fwd_out)
            conv[place, cut(c)] = out
            acc1[place] += fold(out)
            acc2[place] += fold(out * out)
        return carry

    lax.fori_loop(0, chunks, conv_step, 0)

    first_lanes = lax.broadcasted_iota(jnp.int32, (mid, LANES), 1) < LANES // 2
    st1[...] = jnp.where(
        first_lanes,
        jnp.sum(acc1[...], 1, keepdims=True),
        jnp.sum(acc2[...], 1, keepdims=True),
    )
    swap1 = remote(st1, st1_in, tp_send.at[0], tp_recv.at[0], (sp, 1 - tp))
    swap1.start()

    halos[2].wait_recv()
    halos[3].wait_recv()

    def edge_step(c, carry):
        both = jnp.concatenate([go[pl.ds(0, edge)], go[pl.ds(rows + edge, edge)]], 0)
        out = mix(both, w[cut(c)])
        gm[pl.ds(0, edge), cut(c)] = out[:edge]
        gm[pl.ds(rows + edge, edge), cut(c)] = out[edge:]
        return carry

    lax.fori_loop(0, chunks, edge_step, 0)
    loads[7].wait()
    loads[8].wait()
    colg[...] = jnp.zeros_like(colg)
    cols[...] = jnp.zeros_like(cols)
    swap1.wait_recv()
    lanes = lax.broadcasted_iota(jnp.int32, (ALIGN, LANES), 1) < LANES // 2

    def norm_step(i, carry):
        part = pl.ds(pl.multiple_of(i * ALIGN, ALIGN), ALIGN)
        tot = (st1[part] + st1_in[part]) * (1.0 / width)
        mean = tot[:, :1]
        var = tot[:, LANES // 2 : LANES // 2 + 1] - mean * mean
        inv = lax.rsqrt(var + EPS)
        normed = (conv[part] - mean) * inv
        pre = normed * gain[...] + shift[...]
        sig = sigmoid(pre)
        gp = gm[part] * sig * (1.0 + pre * (1.0 - sig))
        gn = gp * gain[...]
        conv[part] = normed
        gm[part] = gn
        gx = gn * normed
        st2[part] = jnp.where(
            lanes,
            jnp.sum(fold(gn), 1, keepdims=True),
            jnp.sum(fold(gx), 1, keepdims=True),
        )
        inv_s[part] = jnp.broadcast_to(inv, (ALIGN, LANES))

        @pl.when((i >= edge // ALIGN) & (i < (rows + edge) // ALIGN))
        def _():
            gpn = gp * normed
            colg[...] += gpn[:8] + gpn[8:]
            cols[...] += gp[:8] + gp[8:]

        return carry

    lax.fori_loop(0, mid // ALIGN, norm_step, 0)
    swap2 = remote(st2, st2_in, tp_send.at[1], tp_recv.at[1], (sp, 1 - tp))
    swap2.start()

    rg = jnp.sum(colg[...], 0, keepdims=True)
    rsh = jnp.sum(cols[...], 0, keepdims=True)
    groups = channels // LANES
    for k in range(groups):
        gs[sp, pl.ds(k, 1), :] = rg[:, k * LANES : (k + 1) * LANES]
        gs[sp, pl.ds(groups + k, 1), :] = rsh[:, k * LANES : (k + 1) * LANES]

    def send_gs(d, carry):
        remote(gs.at[sp], gs.at[sp], all_send.at[0], all_recv.at[0], (peer(d), tp)).start()
        return carry

    lax.fori_loop(1, n, send_gs, 0)
    swap2.wait_recv()

    def gc_step(i, carry):
        part = pl.ds(pl.multiple_of(i * ALIGN, ALIGN), ALIGN)
        tot = (st2[part] + st2_in[part]) * (1.0 / width)
        m1 = tot[:, :1]
        m2 = tot[:, LANES // 2 : LANES // 2 + 1]
        inv = inv_s[part][:, :1]
        gcw[part] = (inv * (gm[part] - m1 - conv[part] * m2)).astype(BF16)
        return carry

    lax.fori_loop(0, mid // ALIGN, gc_step, 0)

    @pl.when(sp == 0)
    def _():
        gcw[pl.ds(0, edge)] = jnp.zeros((edge, channels), BF16)

    @pl.when(sp == n - 1)
    def _():
        gcw[pl.ds(rows + edge, edge)] = jnp.zeros((edge, channels), BF16)

    if n * per > tiles:
        rs_src[pl.ds(tiles, n * per - tiles)] = jnp.zeros(
            (n * per - tiles, ALIGN, LANES), BF16
        )

    def spec_step(c, carry):
        dr = jnp.zeros((freqs, CHUNK), F32)
        di = jnp.zeros((freqs, CHUNK), F32)
        for b in range(2):
            spec = dot(mats[pl.ds(0, size)], gcw[pl.ds(b * plan.bwd_step, size), cut(c)])
            gs_spec[pl.ds(b * size, size), cut(c)] = spec
            re, im = spec[:freqs], spec[freqs:]
            hr = hs[pl.ds(b * size, freqs), cut(c)]
            hi = hs[pl.ds(b * size + freqs, freqs), cut(c)]
            dr = dr + hr * re + hi * im
            di = di + hr * im - hi * re
        prod = jnp.concatenate([dr, di], 0).astype(BF16)
        out = dot(mats[pl.ds(plan.at_lags, plan.tap_rows)], prod) * plan.lag_scale
        out = out.astype(BF16)
        for r in range(plan.tap_rows // ALIGN):
            for k in range(CHUNK // LANES):
                rs_src[r * groups + c * (CHUNK // LANES) + k] = out[
                    r * ALIGN : (r + 1) * ALIGN, k * LANES : (k + 1) * LANES
                ]
        return carry

    lax.fori_loop(0, chunks, spec_step, 0)

    def send_rs(d, carry):
        to = peer(d)
        remote(rs_src.at[pl.ds(to * per, per)], rs_in.at[sp],
               all_send.at[1], all_recv.at[1], (to, tp)).start()
        return carry

    lax.fori_loop(1, n, send_rs, 0)
    rs_in[sp] = rs_src[pl.ds(sp * per, per)]

    def out_step(c, carry):
        ta = ts[pl.ds(0, freqs), cut(c)]
        tb = ts[pl.ds(freqs, freqs), cut(c)]
        for b in range(2):
            re = gs_spec[pl.ds(b * size, freqs), cut(c)]
            im = gs_spec[pl.ds(b * size + freqs, freqs), cut(c)]
            prod = jnp.concatenate([re * ta - im * tb, -(re * tb + im * ta)], 0).astype(BF16)
            out = dot(mats[pl.ds(plan.at_grad + b * plan.bwd_out, plan.bwd_out)], prod)
            place = pl.ds(b * plan.bwd_out, plan.bwd_out)
            sig = sig_s[place, cut(c)]
            left = out * sig
            dv[place, cut(c)] = left.astype(BF16)
            dg[place, cut(c)] = (
                left * value[place, cut(c)].astype(F32) * (1.0 - sig)
            ).astype(BF16)
        return carry

    lax.fori_loop(0, chunks, out_step, 0)
    outs = [
        pltpu.make_async_copy(dv, dv_h, out_sem.at[0]),
        pltpu.make_async_copy(dg, dg_h, out_sem.at[1]),
    ]
    for out in outs:
        out.start()

    def settle(ref, k):
        part = ref.at[pl.ds(0, n - 1)]
        pltpu.make_async_copy(part, part, all_recv.at[k]).wait()

    def settle_sent(ref, k):
        part = ref.at[pl.ds(0, n - 1)]
        pltpu.make_async_copy(part, part, all_send.at[k]).wait()

    settle(rs_in, 1)
    zero = jnp.zeros((per, ALIGN, LANES), F32)
    summed = lax.fori_loop(0, n, lambda i, t: t + rs_in[i].astype(F32), zero)
    ag[sp] = summed.astype(BF16)

    def send_ag(d, carry):
        remote(ag.at[sp], ag.at[sp], all_send.at[2], all_recv.at[2], (peer(d), tp)).start()
        return carry

    lax.fori_loop(1, n, send_ag, 0)

    settle(gs, 0)
    small = lax.fori_loop(
        0, n, lambda i, t: t + gs[i], jnp.zeros(gs.shape[1:], F32)
    )
    dgs_o[...] = small * (1.0 / math.sqrt(total))

    for halo in halos:
        halo.wait_send()
    swap1.wait_send()
    swap2.wait_send()
    settle_sent(gs, 0)
    settle_sent(rs_in, 1)
    settle(ag, 2)
    for t in range(tiles):
        r, k = t // groups, t % groups
        count = min(ALIGN, plan.kernel - r * ALIGN)
        dt_o[pl.ds(r * ALIGN, count), pl.ds(k * LANES, LANES)] = ag[t // per, t % per].astype(F32)[
            :count
        ]
    settle_sent(ag, 2)
    for out in outs:
        out.wait()


def store(*refs):
    sources, targets, holds = refs[:4], refs[4:9], refs[9:13]
    in_sem, out_sem = refs[13:]
    groups = holds[3].shape[0] // 2
    views = list(holds[:3]) + [
        holds[3].at[pl.ds(0, groups)], holds[3].at[pl.ds(groups, groups)]
    ]
    loads = [
        pltpu.make_async_copy(a, b, in_sem.at[i]) for i, (a, b) in enumerate(zip(sources, holds))
    ]
    copies = [
        pltpu.make_async_copy(a, b, out_sem.at[i]) for i, (a, b) in enumerate(zip(views, targets))
    ]
    for load in loads:
        load.start()
    for i, copy in enumerate(copies):
        if i < len(loads):
            loads[i].wait()
        copy.start()
    for copy in copies:
        copy.wait()


def shards(n, value_in, gate_in, taps, gain, shift, w_out, grad_out):
    rows, channels = value_in.shape
    kernel = taps.shape[0]
    total = rows * n
    plan = Plan(rows, kernel, total)
    groups = channels // LANES
    tiles = plan.tap_rows // ALIGN * groups
    per = -(-tiles // n)
    model = grad_out.shape[1]
    mats = jnp.asarray(plan.mats, BF16)
    own = jnp.asarray(plan.own, BF16)
    ft = jnp.asarray(plan.taps, F32)
    hbm = pl.BlockSpec(memory_space=pltpu.HBM)
    vmem = pl.BlockSpec(memory_space=pltpu.VMEM)
    size, mid = plan.size, plan.mid
    chunks = channels // CHUNK
    dma = pltpu.SemaphoreType.DMA
    results = pl.pallas_call(
        functools.partial(body, plan, n, tiles, per, total),
        out_shape=(
            jax.ShapeDtypeStruct((rows, channels), BF16),
            jax.ShapeDtypeStruct((rows, channels), BF16),
            jax.ShapeDtypeStruct((kernel, channels), F32),
            jax.ShapeDtypeStruct((2 * groups, LANES), F32),
        ),
        in_specs=[hbm] * 10,
        out_specs=(hbm, hbm, vmem, vmem),
        scratch_shapes=[
            pltpu.VMEM((rows, channels), BF16),
            pltpu.VMEM((rows, channels), BF16),
            pltpu.VMEM((kernel, channels), F32),
            pltpu.VMEM((1, channels), F32),
            pltpu.VMEM((1, channels), F32),
            pltpu.VMEM((channels, model), BF16),
            pltpu.VMEM((mid, model), BF16),
            pltpu.VMEM(plan.mats.shape, BF16),
            pltpu.VMEM(plan.own.shape, BF16),
            pltpu.VMEM(plan.taps.shape, F32),
            pltpu.VMEM((rows, channels), F32),
            pltpu.VMEM((plan.wide, channels), BF16),
            pltpu.VMEM((mid, channels), F32),
            pltpu.VMEM((mid, channels), F32),
            pltpu.VMEM((mid, channels), BF16),
            pltpu.VMEM((size, channels), F32),
            pltpu.VMEM((2 * size, channels), F32),
            pltpu.VMEM((2 * size, channels), F32),
            pltpu.VMEM((mid, LANES), F32),
            pltpu.VMEM((mid, LANES), F32),
            pltpu.VMEM((mid, LANES), F32),
            pltpu.VMEM((mid, LANES), F32),
            pltpu.VMEM((mid, LANES), F32),
            pltpu.VMEM((mid, LANES), F32),
            pltpu.VMEM((mid, LANES), F32),
            pltpu.VMEM((8, channels), F32),
            pltpu.VMEM((8, channels), F32),
            pltpu.VMEM((n, 2 * groups, LANES), F32),
            pltpu.VMEM((n * per, ALIGN, LANES), BF16),
            pltpu.VMEM((n, per, ALIGN, LANES), BF16),
            pltpu.VMEM((n, per, ALIGN, LANES), BF16),
            pltpu.VMEM((rows, channels), BF16),
            pltpu.VMEM((rows, channels), BF16),
            dma((9,)), dma((chunks,)), dma((2,)), dma((4,)), dma((4,)),
            dma((2,)), dma((2,)), dma((3,)), dma((3,)),
        ],
        compiler_params=pltpu.CompilerParams(
            collective_id=0, has_side_effects=True, vmem_limit_bytes=VMEM_GRANT
        ),
    )(
        value_in, gate_in, taps, gain.reshape(1, -1), shift.reshape(1, -1), w_out,
        grad_out, mats, own, ft,
    )
    d_value, d_gate, d_taps, d_gain, d_shift = pl.pallas_call(
        store,
        out_shape=(
            jax.ShapeDtypeStruct((rows, channels), BF16),
            jax.ShapeDtypeStruct((rows, channels), BF16),
            jax.ShapeDtypeStruct((kernel, channels), F32),
            jax.ShapeDtypeStruct((groups, LANES), F32),
            jax.ShapeDtypeStruct((groups, LANES), F32),
        ),
        in_specs=[hbm] * 4,
        out_specs=(hbm,) * 5,
        scratch_shapes=[
            pltpu.VMEM((rows, channels), BF16),
            pltpu.VMEM((rows, channels), BF16),
            pltpu.VMEM((kernel, channels), F32),
            pltpu.VMEM((2 * groups, LANES), F32),
            dma((4,)), dma((5,)),
        ],
        compiler_params=pltpu.CompilerParams(vmem_limit_bytes=VMEM_GRANT),
    )(*results)
    return (d_value, d_gate, d_taps, d_gain.reshape(-1), d_shift.reshape(-1))


def solution(mesh):
    return jax.shard_map(
        functools.partial(shards, mesh.shape["sp"]),
        mesh=mesh,
        in_specs=(
            P("sp", "tp"),
            P("sp", "tp"),
            P(None, "tp"),
            P("tp"),
            P("tp"),
            P("tp", None),
            P("sp", None),
        ),
        out_specs=(P("sp", "tp"), P("sp", "tp"), P(None, "tp"), P("tp"), P("tp")),
        check_vma=False,
    )
```

```python
import functools
import math

import jax
import jax.numpy as jnp
import numpy as np
from jax import lax
from jax.experimental import pallas as pl
from jax.experimental.pallas import tpu as pltpu
from jax.sharding import PartitionSpec as P

EPS = 1e-05
ALIGN = 16
LANES = 128
CHUNK = 256
VMEM_GRANT = 62 * 1024 * 1024
F32 = jnp.float32
BF16 = jnp.bfloat16


class Plan:
    def __init__(self, rows, kernel, total):
        self.half = kernel // 2
        self.kernel = kernel
        self.rows = rows
        self.edge = -(-(self.half + 1) // ALIGN) * ALIGN
        edge = self.edge
        self.size = rows // 2 + 4 * edge
        size = self.size
        self.freqs = size // 2
        self.wide = rows + 4 * edge
        self.mid = rows + 2 * edge
        self.fwd_out = self.mid // 2
        self.fwd_step = self.wide - size
        self.bwd_out = rows // 2
        self.bwd_step = self.mid - size
        omega = 2.0 * np.pi * (np.arange(self.freqs) + 0.5) / size

        def spectrum(times):
            angle = omega[:, None] * times[None, :]
            return np.concatenate([np.cos(angle), np.sin(angle)], 0)

        def inverse(times):
            angle = times[:, None] * omega[None, :]
            return np.concatenate([np.cos(angle), -np.sin(angle)], 1)

        forward = spectrum(np.arange(size))
        conv = []
        grad = []
        own = []
        for b in range(2):
            start = b * self.fwd_out + edge - self.half - b * self.fwd_step
            conv.append(inverse(np.arange(self.fwd_out) + start))
            start = b * self.bwd_out + edge + self.half - b * self.bwd_step
            grad.append(inverse(np.arange(self.bwd_out) + start))
            start = b * self.bwd_out + edge - b * self.bwd_step
            own.append(spectrum(np.arange(self.bwd_out) + start))
        self.tap_rows = -(-kernel // ALIGN) * ALIGN
        lags = inverse(np.arange(self.tap_rows) - self.half)
        lags[kernel:] = 0.0
        self.mats = np.concatenate([forward] + conv + grad + [lags], 0)
        self.at_conv = size
        self.at_grad = self.at_conv + self.mid
        self.at_lags = self.at_grad + rows
        self.own = np.concatenate(own, 0)
        self.taps = spectrum(np.arange(kernel)) * (2.0 / size)
        self.lag_scale = 2.0 / size / math.sqrt(total)


def dot(a, b):
    return jnp.dot(a, b, preferred_element_type=F32)


def sigmoid(x):
    return 0.5 * jnp.tanh(0.5 * x) + 0.5


def body(
    plan, n, tiles, per, total,
    value_h, gate_h, taps_h, gain_h, shift_h, w_h, go_h, mats_h, own_h, ft_h,
    dv_h, dg_h, dt_o, dgs_o,
    value, gate, taps, gain, shift, w, go, mats, own, ft,
    sig_s, gw, conv, gm, gcw, ts, hs, gs_spec, acc1, acc2,
    st1, st1_in, st2, st2_in, inv_s, colg, cols,
    gs, rs_src, rs_in, ag, dv, dg,
    load_sem, w_sem, out_sem, halo_send, halo_recv, tp_send, tp_recv,
    all_send, all_recv,
):
    sp = lax.axis_index("sp")
    tp = lax.axis_index("tp")
    rows, edge, half2 = plan.rows, plan.edge, 2 * plan.edge
    channels = value.shape[1]
    width = channels * 2
    chunks = channels // CHUNK
    size, freqs, mid = plan.size, plan.freqs, plan.mid
    nxt = lax.rem(sp + 1, n)
    prv = lax.rem(sp + n - 1, n)

    def peer(d):
        return lax.rem(sp + d, n)

    barrier = pltpu.get_barrier_semaphore()

    def greet(d, carry):
        pl.semaphore_signal(
            barrier, 1, device_id=(peer(d), tp), device_id_type=pl.DeviceIdType.MESH
        )
        return carry

    pl.semaphore_signal(
        barrier, 1, device_id=(sp, 1 - tp), device_id_type=pl.DeviceIdType.MESH
    )
    lax.fori_loop(1, n, greet, 0)

    own_go = go.at[pl.ds(edge, rows)]
    pairs = [
        (value_h, value), (gate_h, gate), (taps_h, taps), (ft_h, ft), (own_h, own),
        (mats_h, mats), (go_h, own_go), (gain_h, gain), (shift_h, shift),
    ]
    loads = [
        pltpu.make_async_copy(a, b, load_sem.at[i]) for i, (a, b) in enumerate(pairs)
    ]
    for load in loads:
        load.start()

    def w_copy(c):
        part = pl.ds(pl.multiple_of(c * CHUNK, CHUNK), CHUNK)
        return pltpu.make_async_copy(w_h.at[part], w.at[part], w_sem.at[c])

    for c in range(chunks):
        w_copy(c).start()

    def cut(c):
        return pl.ds(pl.multiple_of(c * CHUNK, CHUNK), CHUNK)

    loads[0].wait()
    loads[1].wait()

    def gate_step(i, carry):
        part = pl.ds(pl.multiple_of(i * ALIGN, ALIGN), ALIGN)
        place = pl.ds(pl.multiple_of(i * ALIGN + half2, ALIGN), ALIGN)
        sig = sigmoid(gate[part].astype(F32))
        sig_s[part] = sig
        gw[place] = (value[part].astype(F32) * sig).astype(BF16)
        return carry

    lax.fori_loop(0, rows // ALIGN, gate_step, 0, unroll=4)
    for load in loads[2:7]:
        load.wait()

    def tap_step(c, carry):
        ts[:, cut(c)] = jnp.dot(
            ft[...], taps[:, cut(c)], precision=lax.Precision.HIGHEST,
            preferred_element_type=F32,
        )
        return carry

    lax.fori_loop(0, chunks, tap_step, 0, unroll=2)

    pl.semaphore_wait(barrier, n)

    def remote(src, dst, send, recv, device):
        return pltpu.make_async_remote_copy(
            src_ref=src, dst_ref=dst, send_sem=send, recv_sem=recv,
            device_id=device, device_id_type=pl.DeviceIdType.MESH,
        )

    halos = [
        remote(gw.at[pl.ds(rows, half2)], gw.at[pl.ds(0, half2)],
               halo_send.at[0], halo_recv.at[0], (nxt, tp)),
        remote(gw.at[pl.ds(half2, half2)], gw.at[pl.ds(rows + half2, half2)],
               halo_send.at[1], halo_recv.at[1], (prv, tp)),
        remote(go.at[pl.ds(rows, edge)], go.at[pl.ds(0, edge)],
               halo_send.at[2], halo_recv.at[2], (nxt, tp)),
        remote(go.at[pl.ds(edge, edge)], go.at[pl.ds(rows + edge, edge)],
               halo_send.at[3], halo_recv.at[3], (prv, tp)),
    ]
    for halo in halos:
        halo.start()

    def mix(a, b):
        return lax.dot_general(a, b, (((1,), (1,)), ((), ())), preferred_element_type=F32)

    def own_step(c, carry):
        for b in range(2):
            hs[pl.ds(b * size, size), cut(c)] = dot(
                own[pl.ds(b * size, size)],
                gw[pl.ds(half2 + b * plan.bwd_out, plan.bwd_out), cut(c)],
            )
        return carry

    lax.fori_loop(0, chunks, own_step, 0, unroll=2)

    def mix_step(c, carry):
        w_copy(c).wait()
        gm[pl.ds(edge, rows), cut(c)] = mix(go[pl.ds(edge, rows)], w[cut(c)])
        return carry

    lax.fori_loop(0, chunks, mix_step, 0)

    halos[0].wait_recv()
    halos[1].wait_recv()

    @pl.when(sp == 0)
    def _():
        gw[pl.ds(0, half2)] = jnp.zeros((half2, channels), BF16)

    @pl.when(sp == n - 1)
    def _():
        gw[pl.ds(rows + half2, half2)] = jnp.zeros((half2, channels), BF16)

    acc1[...] = jnp.zeros_like(acc1)
    acc2[...] = jnp.zeros_like(acc2)

    def fold(x):
        out = x[:, :LANES]
        for k in range(1, x.shape[1] // LANES):
            out = out + x[:, k * LANES : (k + 1) * LANES]
        return out

    def conv_step(c, carry):
        ta = ts[pl.ds(0, freqs), cut(c)]
        tb = ts[pl.ds(freqs, freqs), cut(c)]
        for b in range(2):
            spec = dot(mats[pl.ds(0, size)], gw[pl.ds(b * plan.fwd_step, size), cut(c)])
            re, im = spec[:freqs], spec[freqs:]
            prod = jnp.concatenate([re * ta + im * tb, re * tb - im * ta], 0).astype(BF16)
            out = dot(mats[pl.ds(plan.at_conv + b * plan.fwd_out, plan.fwd_out)], prod)
            place = pl.ds(b * plan.fwd_out, plan.fwd_out)
            conv[place, cut(c)] = out
            acc1[place] += fold(out)
            acc2[place] += fold(out * out)
        return carry

    lax.fori_loop(0, chunks, conv_step, 0, unroll=2)

    first_lanes = lax.broadcasted_iota(jnp.int32, (mid, LANES), 1) < LANES // 2
    st1[...] = jnp.where(
        first_lanes,
        jnp.sum(acc1[...], 1, keepdims=True),
        jnp.sum(acc2[...], 1, keepdims=True),
    )
    swap1 = remote(st1, st1_in, tp_send.at[0], tp_recv.at[0], (sp, 1 - tp))
    swap1.start()

    halos[2].wait_recv()
    halos[3].wait_recv()

    def edge_step(c, carry):
        both = jnp.concatenate([go[pl.ds(0, edge)], go[pl.ds(rows + edge, edge)]], 0)
        out = mix(both, w[cut(c)])
        gm[pl.ds(0, edge), cut(c)] = out[:edge]
        gm[pl.ds(rows + edge, edge), cut(c)] = out[edge:]
        return carry

    lax.fori_loop(0, chunks, edge_step, 0)
    loads[7].wait()
    loads[8].wait()
    colg[...] = jnp.zeros_like(colg)
    cols[...] = jnp.zeros_like(cols)
    swap1.wait_recv()
    lanes = lax.broadcasted_iota(jnp.int32, (ALIGN, LANES), 1) < LANES // 2

    def norm_step(i, carry):
        part = pl.ds(pl.multiple_of(i * ALIGN, ALIGN), ALIGN)
        tot = (st1[part] + st1_in[part]) * (1.0 / width)
        mean = tot[:, :1]
        var = tot[:, LANES // 2 : LANES // 2 + 1] - mean * mean
        inv = lax.rsqrt(var + EPS)
        normed = (conv[part] - mean) * inv
        pre = normed * gain[...] + shift[...]
        sig = sigmoid(pre)
        gp = gm[part] * sig * (1.0 + pre * (1.0 - sig))
        gn = gp * gain[...]
        conv[part] = normed
        gm[part] = gn
        gx = gn * normed
        st2[part] = jnp.where(
            lanes,
            jnp.sum(fold(gn), 1, keepdims=True),
            jnp.sum(fold(gx), 1, keepdims=True),
        )
        inv_s[part] = jnp.broadcast_to(inv, (ALIGN, LANES))

        inside = (i >= edge // ALIGN) & (i < (rows + edge) // ALIGN)
        gpn = gp * normed
        colg[...] += jnp.where(inside, gpn[:8] + gpn[8:], 0.0)
        cols[...] += jnp.where(inside, gp[:8] + gp[8:], 0.0)
        return carry

    lax.fori_loop(0, mid // ALIGN, norm_step, 0, unroll=3)
    swap2 = remote(st2, st2_in, tp_send.at[1], tp_recv.at[1], (sp, 1 - tp))
    swap2.start()

    rg = jnp.sum(colg[...], 0, keepdims=True)
    rsh = jnp.sum(cols[...], 0, keepdims=True)
    groups = channels // LANES
    for k in range(groups):
        gs[sp, pl.ds(k, 1), :] = rg[:, k * LANES : (k + 1) * LANES]
        gs[sp, pl.ds(groups + k, 1), :] = rsh[:, k * LANES : (k + 1) * LANES]

    def send_gs(d, carry):
        remote(gs.at[sp], gs.at[sp], all_send.at[0], all_recv.at[0], (peer(d), tp)).start()
        return carry

    lax.fori_loop(1, n, send_gs, 0)
    swap2.wait_recv()

    def gc_step(i, carry):
        part = pl.ds(pl.multiple_of(i * ALIGN, ALIGN), ALIGN)
        tot = (st2[part] + st2_in[part]) * (1.0 / width)
        m1 = tot[:, :1]
        m2 = tot[:, LANES // 2 : LANES // 2 + 1]
        inv = inv_s[part][:, :1]
        gcw[part] = (inv * (gm[part] - m1 - conv[part] * m2)).astype(BF16)
        return carry

    lax.fori_loop(0, mid // ALIGN, gc_step, 0, unroll=6)

    @pl.when(sp == 0)
    def _():
        gcw[pl.ds(0, edge)] = jnp.zeros((edge, channels), BF16)

    @pl.when(sp == n - 1)
    def _():
        gcw[pl.ds(rows + edge, edge)] = jnp.zeros((edge, channels), BF16)

    if n * per > tiles:
        rs_src[pl.ds(tiles, n * per - tiles)] = jnp.zeros(
            (n * per - tiles, ALIGN, LANES), BF16
        )

    def spec_step(c, carry):
        dr = jnp.zeros((freqs, CHUNK), F32)
        di = jnp.zeros((freqs, CHUNK), F32)
        for b in range(2):
            spec = dot(mats[pl.ds(0, size)], gcw[pl.ds(b * plan.bwd_step, size), cut(c)])
            gs_spec[pl.ds(b * size, size), cut(c)] = spec
            re, im = spec[:freqs], spec[freqs:]
            hr = hs[pl.ds(b * size, freqs), cut(c)]
            hi = hs[pl.ds(b * size + freqs, freqs), cut(c)]
            dr = dr + hr * re + hi * im
            di = di + hr * im - hi * re
        prod = jnp.concatenate([dr, di], 0).astype(BF16)
        out = dot(mats[pl.ds(plan.at_lags, plan.tap_rows)], prod) * plan.lag_scale
        out = out.astype(BF16)
        for r in range(plan.tap_rows // ALIGN):
            for k in range(CHUNK // LANES):
                rs_src[r * groups + c * (CHUNK // LANES) + k] = out[
                    r * ALIGN : (r + 1) * ALIGN, k * LANES : (k + 1) * LANES
                ]
        return carry

    lax.fori_loop(0, chunks, spec_step, 0, unroll=2)

    def send_rs(d, carry):
        to = peer(d)
        remote(rs_src.at[pl.ds(to * per, per)], rs_in.at[sp],
               all_send.at[1], all_recv.at[1], (to, tp)).start()
        return carry

    lax.fori_loop(1, n, send_rs, 0)
    rs_in[sp] = rs_src[pl.ds(sp * per, per)]

    def out_step(c, carry):
        ta = ts[pl.ds(0, freqs), cut(c)]
        tb = ts[pl.ds(freqs, freqs), cut(c)]
        for b in range(2):
            re = gs_spec[pl.ds(b * size, freqs), cut(c)]
            im = gs_spec[pl.ds(b * size + freqs, freqs), cut(c)]
            prod = jnp.concatenate([re * ta - im * tb, -(re * tb + im * ta)], 0).astype(BF16)
            out = dot(mats[pl.ds(plan.at_grad + b * plan.bwd_out, plan.bwd_out)], prod)
            place = pl.ds(b * plan.bwd_out, plan.bwd_out)
            sig = sig_s[place, cut(c)]
            left = out * sig
            dv[place, cut(c)] = left.astype(BF16)
            dg[place, cut(c)] = (
                left * value[place, cut(c)].astype(F32) * (1.0 - sig)
            ).astype(BF16)
        return carry

    lax.fori_loop(0, chunks, out_step, 0, unroll=2)
    outs = [
        pltpu.make_async_copy(dv, dv_h, out_sem.at[0]),
        pltpu.make_async_copy(dg, dg_h, out_sem.at[1]),
    ]
    for out in outs:
        out.start()

    def settle(ref, k):
        part = ref.at[pl.ds(0, n - 1)]
        pltpu.make_async_copy(part, part, all_recv.at[k]).wait()

    def settle_sent(ref, k):
        part = ref.at[pl.ds(0, n - 1)]
        pltpu.make_async_copy(part, part, all_send.at[k]).wait()

    settle(rs_in, 1)
    zero = jnp.zeros((per, ALIGN, LANES), F32)
    summed = lax.fori_loop(0, n, lambda i, t: t + rs_in[i].astype(F32), zero)
    ag[sp] = summed.astype(BF16)

    def send_ag(d, carry):
        remote(ag.at[sp], ag.at[sp], all_send.at[2], all_recv.at[2], (peer(d), tp)).start()
        return carry

    lax.fori_loop(1, n, send_ag, 0)

    settle(gs, 0)
    small = lax.fori_loop(
        0, n, lambda i, t: t + gs[i], jnp.zeros(gs.shape[1:], F32)
    )
    dgs_o[...] = small * (1.0 / math.sqrt(total))

    for halo in halos:
        halo.wait_send()
    swap1.wait_send()
    swap2.wait_send()
    settle_sent(gs, 0)
    settle_sent(rs_in, 1)
    settle(ag, 2)
    for t in range(tiles):
        r, k = t // groups, t % groups
        count = min(ALIGN, plan.kernel - r * ALIGN)
        dt_o[pl.ds(r * ALIGN, count), pl.ds(k * LANES, LANES)] = ag[t // per, t % per].astype(F32)[
            :count
        ]
    settle_sent(ag, 2)
    for out in outs:
        out.wait()


def store(*refs):
    sources, targets, holds = refs[:4], refs[4:9], refs[9:13]
    in_sem, out_sem = refs[13:]
    groups = holds[3].shape[0] // 2
    views = list(holds[:3]) + [
        holds[3].at[pl.ds(0, groups)], holds[3].at[pl.ds(groups, groups)]
    ]
    loads = [
        pltpu.make_async_copy(a, b, in_sem.at[i]) for i, (a, b) in enumerate(zip(sources, holds))
    ]
    copies = [
        pltpu.make_async_copy(a, b, out_sem.at[i]) for i, (a, b) in enumerate(zip(views, targets))
    ]
    for load in loads:
        load.start()
    for i, copy in enumerate(copies):
        if i < len(loads):
            loads[i].wait()
        copy.start()
    for copy in copies:
        copy.wait()


def shards(n, value_in, gate_in, taps, gain, shift, w_out, grad_out):
    rows, channels = value_in.shape
    kernel = taps.shape[0]
    total = rows * n
    plan = Plan(rows, kernel, total)
    groups = channels // LANES
    tiles = plan.tap_rows // ALIGN * groups
    per = -(-tiles // n)
    model = grad_out.shape[1]
    mats = jnp.asarray(plan.mats, BF16)
    own = jnp.asarray(plan.own, BF16)
    ft = jnp.asarray(plan.taps, F32)
    hbm = pl.BlockSpec(memory_space=pltpu.HBM)
    vmem = pl.BlockSpec(memory_space=pltpu.VMEM)
    size, mid = plan.size, plan.mid
    chunks = channels // CHUNK
    dma = pltpu.SemaphoreType.DMA
    results = pl.pallas_call(
        functools.partial(body, plan, n, tiles, per, total),
        out_shape=(
            jax.ShapeDtypeStruct((rows, channels), BF16),
            jax.ShapeDtypeStruct((rows, channels), BF16),
            jax.ShapeDtypeStruct((kernel, channels), F32),
            jax.ShapeDtypeStruct((2 * groups, LANES), F32),
        ),
        in_specs=[hbm] * 10,
        out_specs=(hbm, hbm, vmem, vmem),
        scratch_shapes=[
            pltpu.VMEM((rows, channels), BF16),
            pltpu.VMEM((rows, channels), BF16),
            pltpu.VMEM((kernel, channels), F32),
            pltpu.VMEM((1, channels), F32),
            pltpu.VMEM((1, channels), F32),
            pltpu.VMEM((channels, model), BF16),
            pltpu.VMEM((mid, model), BF16),
            pltpu.VMEM(plan.mats.shape, BF16),
            pltpu.VMEM(plan.own.shape, BF16),
            pltpu.VMEM(plan.taps.shape, F32),
            pltpu.VMEM((rows, channels), F32),
            pltpu.VMEM((plan.wide, channels), BF16),
            pltpu.VMEM((mid, channels), F32),
            pltpu.VMEM((mid, channels), F32),
            pltpu.VMEM((mid, channels), BF16),
            pltpu.VMEM((size, channels), F32),
            pltpu.VMEM((2 * size, channels), F32),
            pltpu.VMEM((2 * size, channels), F32),
            pltpu.VMEM((mid, LANES), F32),
            pltpu.VMEM((mid, LANES), F32),
            pltpu.VMEM((mid, LANES), F32),
            pltpu.VMEM((mid, LANES), F32),
            pltpu.VMEM((mid, LANES), F32),
            pltpu.VMEM((mid, LANES), F32),
            pltpu.VMEM((mid, LANES), F32),
            pltpu.VMEM((8, channels), F32),
            pltpu.VMEM((8, channels), F32),
            pltpu.VMEM((n, 2 * groups, LANES), F32),
            pltpu.VMEM((n * per, ALIGN, LANES), BF16),
            pltpu.VMEM((n, per, ALIGN, LANES), BF16),
            pltpu.VMEM((n, per, ALIGN, LANES), BF16),
            pltpu.VMEM((rows, channels), BF16),
            pltpu.VMEM((rows, channels), BF16),
            dma((9,)), dma((chunks,)), dma((2,)), dma((4,)), dma((4,)),
            dma((2,)), dma((2,)), dma((3,)), dma((3,)),
        ],
        compiler_params=pltpu.CompilerParams(
            collective_id=0, has_side_effects=True, vmem_limit_bytes=VMEM_GRANT
        ),
    )(
        value_in, gate_in, taps, gain.reshape(1, -1), shift.reshape(1, -1), w_out,
        grad_out, mats, own, ft,
    )
    d_value, d_gate, d_taps, d_gain, d_shift = pl.pallas_call(
        store,
        out_shape=(
            jax.ShapeDtypeStruct((rows, channels), BF16),
            jax.ShapeDtypeStruct((rows, channels), BF16),
            jax.ShapeDtypeStruct((kernel, channels), F32),
            jax.ShapeDtypeStruct((groups, LANES), F32),
            jax.ShapeDtypeStruct((groups, LANES), F32),
        ),
        in_specs=[hbm] * 4,
        out_specs=(hbm,) * 5,
        scratch_shapes=[
            pltpu.VMEM((rows, channels), BF16),
            pltpu.VMEM((rows, channels), BF16),
            pltpu.VMEM((kernel, channels), F32),
            pltpu.VMEM((2 * groups, LANES), F32),
            dma((4,)), dma((5,)),
        ],
        compiler_params=pltpu.CompilerParams(vmem_limit_bytes=VMEM_GRANT),
    )(*results)
    return (d_value, d_gate, d_taps, d_gain.reshape(-1), d_shift.reshape(-1))


def solution(mesh):
    return jax.shard_map(
        functools.partial(shards, mesh.shape["sp"]),
        mesh=mesh,
        in_specs=(
            P("sp", "tp"),
            P("sp", "tp"),
            P(None, "tp"),
            P("tp"),
            P("tp"),
            P("tp", None),
            P("sp", None),
        ),
        out_specs=(P("sp", "tp"), P("sp", "tp"), P(None, "tp"), P("tp"), P("tp")),
        check_vma=False,
    )
```
